32 devices in a mesh: sp: 16 (over z, y, x), tp: 2 (over core).
Axes of the slice: x: 2, y: 2, z: 4, core: 2. Of those that a mesh axis runs over, the one named last changes fastest.
Arguments:
- stream: bfloat16 [8192, 2048], P(('sp', 'tp')), may hold values from -6 to 6
- queries: bfloat16 [8192, 512], P('sp', 'tp'), may hold values from -6 to 6
- key_rows: bfloat16 [8192, 512], P('sp', 'tp'), may hold values from -6 to 6
- value_rows: bfloat16 [8192, 1024], P('sp', 'tp'), may hold values from -6 to 6
- out_gate: bfloat16 [8192, 1024], P('sp', 'tp'), may hold values from -6 to 6
- in_gate: float32 [4, 8192], P('tp', 'sp'), may hold values from -4 to 214
- forget_gate: float32 [4, 8192], P('tp', 'sp'), may hold values from -2 to 20
- out_proj: bfloat16 [1024, 2048], replicated, may hold values from -0.1875 to 0.1875
- ffn_gain: float32 [2048], replicated, may hold values from 0.1 to 1.9
- gate_proj: bfloat16 [16, 2048, 768], P('sp', None, 'tp'), may hold values from -0.125 to 0.125
- up_proj: bfloat16 [16, 2048, 768], P('sp', None, 'tp'), may hold values from -0.125 to 0.125
- down_proj: bfloat16 [16, 768, 2048], P('sp', 'tp'), may hold values from -0.21875 to 0.21875
- expert_ids: int32 [8192, 2], P(('sp', 'tp')), may hold values from 0 to 15, as said below
- route_weights: float32 [8192, 2], P(('sp', 'tp')), may hold values from 0.05 to 1
Outputs:
- result_stream: bfloat16 [8192, 2048], P(('sp', 'tp'))
The draws below stay inside these ranges and needn't reach their ends.
Inputs may be any that keep to these rules, and one draw needn't show every extreme that they name: `expert_ids`: both experts of a row are different and lie in one group (expert // 8 equal). In the rows of one device (aligned blocks of 256 rows) each expert is named at most 64 times, some expert exactly 64 times, and each expert shares its rows with a single partner.
All inputs are finite; a program needn't handle non-finite values.
Results may differ from the reference program's by a relative error of at most 0.012.
Values may be sent and summed in bfloat16 or wider, within the bound.
A program may use at most 128 MiB of HBM per device.

```python
import jax
import jax.numpy as jnp
from jax import lax

D = 2048
HEADS = 4
QK = 128
V_DIM = 256
FF = 768
GROUP = 8
TOPK = 2
BLOCK = 64
TOK_DEV = 512
TOKENS = 8192
EXPERTS = 16
ROWS = 256
CAP = 64
N_SP = 16
N_TP = 2


def draw_in_gate(key, part):
    base = jnp.clip(jax.random.normal(jax.random.fold_in(key, 3), (HEADS, TOKENS), jnp.float32), -4.0, 4.0)
    return base


def draw_forget_gate(key, part):
    order_key = jax.random.fold_in(key, 5)
    device_key = jax.random.fold_in(key, 6)
    block_key = jax.random.fold_in(key, 7)
    noise_key = jax.random.fold_in(key, 8)
    order = jax.random.permutation(order_key, HEADS)
    quick = order < HEADS // 2
    base = jnp.where(quick, 1.0 / 40.0, 0.5 / TOKENS).astype(jnp.float32)
    device_factor = jnp.exp(jax.random.uniform(device_key, (HEADS, TOKENS // TOK_DEV), jnp.float32, jnp.log(0.4), jnp.log(2.5)))
    block_factor = jnp.exp(jax.random.uniform(block_key, (HEADS, TOKENS // BLOCK), jnp.float32, jnp.log(0.7), jnp.log(1.4)))
    noise = jnp.clip(jax.random.normal(noise_key, (HEADS, TOKENS), jnp.float32), -3.0, 3.0)
    rate = base[:, None] * jnp.repeat(device_factor, TOK_DEV, axis=1) * jnp.repeat(block_factor, BLOCK, axis=1) * jnp.exp(0.5 * noise)
    return -jnp.log(rate)


def route_table(key):
    groups = EXPERTS // GROUP
    pairs = EXPERTS // 2
    slot_total = pairs * CAP
    star_key = jax.random.fold_in(key, 21)
    share_key = jax.random.fold_in(key, 22)
    blocks_key = jax.random.fold_in(key, 23)
    star = jax.random.randint(star_key, (), 0, EXPERTS)
    shared = jax.random.randint(share_key, (EXPERTS,), 0, 3)

    def one_block(block_key):
        pair_key, prio_key, tie_key, shuffle_key, flip_key = jax.random.split(block_key, 5)
        group_keys = jax.random.split(pair_key, groups)
        perms = jax.vmap(lambda group_key: jax.random.permutation(group_key, GROUP))(group_keys)
        members = perms + (jnp.arange(groups, dtype=jnp.int32) * GROUP)[:, None]
        first = members[:, 0::2].reshape(-1)
        second = members[:, 1::2].reshape(-1)
        priority = jnp.maximum(shared[first], shared[second]) + jax.random.randint(prio_key, (pairs,), 0, 3)
        priority = jnp.where((first == star) | (second == star), 100, priority)
        tie = jax.random.permutation(tie_key, slot_total)
        score = priority[jnp.arange(slot_total) // CAP] * slot_total + tie
        _, chosen = lax.top_k(score, ROWS)
        chosen = jax.random.permutation(shuffle_key, chosen)
        pair = chosen // CAP
        flip = jax.random.randint(flip_key, (ROWS,), 0, 2)
        left = first[pair]
        right = second[pair]
        return jnp.stack([jnp.where(flip == 1, right, left), jnp.where(flip == 1, left, right)], axis=1)
    table = jax.vmap(one_block)(jax.random.split(blocks_key, TOKENS // ROWS))
    return table.reshape(TOKENS, 2).astype(jnp.int32)


def draw_expert_ids(key, part):
    return route_table(jax.random.fold_in(key, 11))


def level_of(stream_key, dims, shards, low, high):
    def one(dim, parts):
        heights = jax.random.uniform(jax.random.fold_in(jax.random.fold_in(stream_key, 6), dim), (parts,), jnp.float32, low / len(shards), high / len(shards))
        return jnp.repeat(jnp.exp(heights), dims[dim] // parts).reshape((-1,) + (1,) * (len(dims) - dim - 1))

    gain = one(*shards[0])
    for cut in shards[1:]:
        gain = gain * one(*cut)
    return gain


def bell_draw(rng, shape, scale, most, shards=(), kind=jnp.bfloat16):
    values = scale * jax.random.normal(rng, shape, jnp.float32)
    if shards:
        values = values * level_of(rng, shape, shards, -0.22, 0.18)
    return jnp.clip(values, -most, most).astype(kind)


def setup_inputs(seed: int = 0) -> dict:
    keys = jax.random.split(jax.random.key(seed), 15)
    return {
        "stream": bell_draw(keys[0], (TOKENS, D), 1.0, 6.0, ((0, 32),)),
        "queries": bell_draw(keys[1], (TOKENS, HEADS * QK), 1.0, 6.0, ((0, 16), (1, 2))),
        "key_rows": bell_draw(keys[2], (TOKENS, HEADS * QK), 1.0, 6.0, ((0, 16), (1, 2))),
        "value_rows": bell_draw(keys[3], (TOKENS, HEADS * V_DIM), 1.0, 6.0, ((0, 16), (1, 2))),
        "out_gate": bell_draw(keys[4], (TOKENS, HEADS * V_DIM), 1.0, 6.0, ((0, 16), (1, 2))),
        "in_gate": draw_in_gate(jax.random.fold_in(keys[14], 71), 0),
        "forget_gate": draw_forget_gate(jax.random.fold_in(keys[14], 71), 0),
        "out_proj": bell_draw(keys[7], (HEADS * V_DIM, D), (HEADS * V_DIM) ** -0.5, 0.1875),
        "ffn_gain": jnp.clip(1.0 + 0.18 * jax.random.normal(keys[8], (D,), jnp.float32), 0.1, 1.9),
        "gate_proj": bell_draw(keys[9], (EXPERTS, D, FF), D ** -0.5, 0.125, ((0, 16), (2, 2))),
        "up_proj": bell_draw(keys[10], (EXPERTS, D, FF), D ** -0.5, 0.125, ((0, 16), (2, 2))),
        "down_proj": bell_draw(keys[11], (EXPERTS, FF, D), FF ** -0.5, 0.21875, ((0, 16), (1, 2))),
        "expert_ids": draw_expert_ids(jax.random.fold_in(keys[14], 71), 0),
        "route_weights": jnp.clip(0.05 + 0.95 * jax.random.uniform(keys[13], (TOKENS, TOPK), jnp.float32) ** level_of(keys[13], (TOKENS, TOPK), ((0, 32),), -0.2, 0.2), 0.05, 1.0),
    }


epsilon = 1e-06

def mechanism(queries, key_rows, value_rows, in_gate, forget_gate):
    heads, length = in_gate.shape
    blocks = length // BLOCK

    def per_head(rows, size):
        return rows.astype(jnp.float32).reshape(blocks, BLOCK, heads, size).transpose(2, 0, 1, 3)
    query_blocks = per_head(queries, QK)
    key_blocks = per_head(key_rows, QK) * QK ** (-0.5)
    value_blocks = per_head(value_rows, V_DIM)
    input_gate = in_gate.reshape(heads, blocks, BLOCK)
    cumulative = jnp.cumsum(jax.nn.log_sigmoid(forget_gate).reshape(heads, blocks, BLOCK), axis=-1)
    closing = cumulative[..., -1]
    causal = jnp.tril(jnp.ones((BLOCK, BLOCK), dtype=bool))
    log_inner = jnp.where(causal, cumulative[..., :, None] - cumulative[..., None, :] + input_gate[..., None, :], -jnp.inf)
    log_close = closing[..., None] - cumulative + input_gate

    def advance(carry, inputs):
        state, level = carry
        key_block, value_block, close_block, last_block = inputs
        new_level = jnp.maximum(last_block + level, lax.optimization_barrier(jnp.max(close_block, axis=-1)))
        weight = jnp.exp(close_block - new_level[:, None])
        update = jnp.einsum('hl,hld,hle->hde', weight, key_block, value_block, precision=lax.Precision.HIGHEST)
        new_state = state * jnp.exp(last_block + level - new_level)[:, None, None] + update
        return ((new_state, new_level), (state, level))
    start = (jnp.zeros((heads, QK, V_DIM), jnp.float32), jnp.zeros((heads,), jnp.float32))
    _, (states, levels) = lax.scan(advance, start, (jnp.moveaxis(key_blocks, 1, 0), jnp.moveaxis(value_blocks, 1, 0), jnp.moveaxis(log_close, 1, 0), closing.T))
    states = jnp.moveaxis(states, 0, 1)
    levels = levels.T
    log_inter = cumulative + levels[..., None]
    peak = jnp.maximum(log_inter, lax.optimization_barrier(jnp.max(log_inner, axis=-1)))
    scores = jnp.einsum('hntd,hnsd->hnts', query_blocks, key_blocks, precision=lax.Precision.HIGHEST) * jnp.exp(log_inner - peak[..., None])
    carried = jnp.einsum('hntd,hnde->hnte', query_blocks, states, precision=lax.Precision.HIGHEST)
    local = jnp.einsum('hnts,hnse->hnte', scores, value_blocks, precision=lax.Precision.HIGHEST)
    numerator = jnp.exp(log_inter - peak)[..., None] * carried + local
    return numerator.transpose(1, 2, 0, 3).reshape(length, heads, V_DIM)

def reference(stream, queries, key_rows, value_rows, out_gate, in_gate, forget_gate, out_proj, ffn_gain, gate_proj, up_proj, down_proj, expert_ids, route_weights):
    numerator = mechanism(queries, key_rows, value_rows, in_gate, forget_gate)
    length, heads, _ = numerator.shape
    scaled = numerator * lax.rsqrt(lax.optimization_barrier(jnp.mean(numerator * numerator, axis=-1, keepdims=True)) + epsilon)
    gated = scaled.reshape(length, heads * V_DIM) * jax.nn.sigmoid(out_gate.astype(jnp.float32))
    heads_out = gated.astype(jnp.bfloat16)
    mix = jnp.dot(heads_out, out_proj, preferred_element_type=jnp.float32)
    middle = (stream.astype(jnp.float32) + mix).astype(jnp.bfloat16)
    middle_float = middle.astype(jnp.float32)
    normed = (middle_float * lax.rsqrt(lax.optimization_barrier(jnp.mean(middle_float * middle_float, axis=-1, keepdims=True)) + epsilon) * ffn_gain.astype(jnp.float32)).astype(jnp.bfloat16)
    flat_ids = expert_ids.reshape(-1).astype(jnp.int32)
    flat_weights = route_weights.reshape(-1).astype(jnp.float32)
    flat_tokens = (jnp.arange(TOKENS * TOPK, dtype=jnp.int32) // TOPK).astype(jnp.int32)
    most = N_SP * N_TP * CAP

    def expert_step(total, inputs):
        gate_weight, up_weight, down_weight, index = inputs
        chosen = jnp.nonzero(flat_ids == index, size=most, fill_value=0)[0].astype(jnp.int32)
        amount = jnp.sum((flat_ids == index).astype(jnp.int32))
        live = (jnp.arange(most, dtype=jnp.int32) < amount).astype(jnp.float32)
        owners = flat_tokens[chosen]
        rows = normed[owners]
        hidden = (jax.nn.silu(jnp.dot(rows, gate_weight, preferred_element_type=jnp.float32)) * jnp.dot(rows, up_weight, preferred_element_type=jnp.float32)).astype(jnp.bfloat16)
        output = jnp.dot(hidden, down_weight, preferred_element_type=jnp.float32).astype(jnp.bfloat16).astype(jnp.float32)
        contribution = output * (flat_weights[chosen] * live)[:, None]
        return (total.at[owners].add(contribution), None)
    total, _ = lax.scan(expert_step, jnp.zeros((TOKENS, D), jnp.float32), (gate_proj, up_proj, down_proj, jnp.arange(EXPERTS, dtype=jnp.int32)))
    return (middle_float + total).astype(jnp.bfloat16)
```

```python
import functools

import jax
import jax.numpy as jnp
from jax import lax
from jax.experimental import pallas as pl
from jax.experimental.pallas import tpu as pltpu
from jax.sharding import PartitionSpec as P

GROUP = 8
CUM = 64
epsilon = 1e-06
bf16, f32 = jnp.bfloat16, jnp.float32


def exchange_kernel(axis, group, count, kinds, *refs):
    ins, outs = refs[:count], refs[count : 2 * count]
    send, recv = refs[2 * count :]
    mine = lax.axis_index(axis)
    base = (mine // group) * group
    me = mine - base

    barrier = pltpu.get_barrier_semaphore()
    for step in range(1, group):
        peer = base + lax.rem(me + step, group)
        pl.semaphore_signal(barrier, inc=1, device_id={axis: peer}, device_id_type=pl.DeviceIdType.MESH)
    pl.semaphore_wait(barrier, group - 1)
    copies = []
    for step in range(1, group):
        to = lax.rem(me + step, group)
        for n in range(count):
            copy = pltpu.make_async_remote_copy(
                src_ref=ins[n].at[to] if kinds[n] == "slab" else ins[n],
                dst_ref=outs[n].at[me],
                send_sem=send.at[n, step],
                recv_sem=recv.at[n, step],
                device_id={axis: base + to},
                device_id_type=pl.DeviceIdType.MESH,
            )
            copy.start()
            copies.append(copy)
    for n in range(count):
        outs[n][me] = ins[n][me] if kinds[n] == "slab" else ins[n][...]
    for copy in copies:
        copy.wait()


def exchange(arrays, kinds, axis, group, collective_id, cost):
    count = len(arrays)
    out_shape = [
        jax.ShapeDtypeStruct(a.shape if kind == "slab" else (group,) + a.shape, a.dtype)
        for a, kind in zip(arrays, kinds)
    ]
    return pl.pallas_call(
        functools.partial(exchange_kernel, axis, group, count, kinds),
        out_shape=out_shape,
        in_specs=[pl.BlockSpec(memory_space=pltpu.VMEM)] * count,
        out_specs=[pl.BlockSpec(memory_space=pltpu.VMEM)] * count,
        scratch_shapes=[
            pltpu.SemaphoreType.DMA((count, group)),
            pltpu.SemaphoreType.DMA((count, group)),
        ],
        compiler_params=pltpu.CompilerParams(collective_id=collective_id, has_side_effects=True),
        cost_estimate=pl.CostEstimate(flops=0, bytes_accessed=cost, transcendentals=0),
    )(*arrays)


def device_prefix(state, level, decay):
    total, mine = lax.axis_size("sp"), lax.axis_index("sp")
    heads, qk, width = state.shape
    rows = heads * qk // total
    slabs = state.astype(bf16).reshape(total, rows, width)
    info = jnp.zeros((8, 128), f32).at[0, :heads].set(level).at[1, :heads].set(decay)
    slabs, infos = exchange((slabs, info), ("slab", "all"), "sp", total, 1, 10_000_000)
    levels, decays = infos[:, 0, :heads].T, infos[:, 1, :heads].T
    order = jnp.arange(total)
    between = (order[None, :, None] < order[None, None, :]) & (order[None, None, :] < order[:, None, None])
    gap = jnp.sum(jnp.where(between[None], decays[:, None, None, :], 0.0), axis=-1)
    earlier = order[None, :] < order[:, None]
    reach = jnp.where(earlier[None], levels[:, None, :] + gap, -jnp.inf)
    start = jnp.sum(jnp.where(earlier[None], decays[:, None, :], 0.0), axis=-1)
    top = jnp.maximum(start, jnp.max(reach, axis=-1))
    weights = jnp.exp(reach - top[..., None])
    head_here = mine * heads // total
    weight = lax.dynamic_index_in_dim(weights, head_here, 0, keepdims=False)
    prefix = jnp.dot(
        weight, slabs.astype(f32).reshape(total, rows * width), precision=lax.Precision.HIGHEST
    )
    prefix = prefix.astype(bf16).reshape(total, rows, width)
    (prefix,) = exchange((prefix,), ("slab",), "sp", total, 2, 10_000_000)
    top_mine = lax.dynamic_index_in_dim(top, mine, 1, keepdims=False)
    return prefix.reshape(heads, qk, width), top_mine


def mixer(queries, key_rows, value_rows, out_gate, in_gate, forget_gate):
    heads, length = in_gate.shape
    qk, width = queries.shape[1] // heads, value_rows.shape[1] // heads
    scale = qk ** (-0.5)
    q = queries.reshape(length, heads, qk)
    k = key_rows.reshape(length, heads, qk)
    v = value_rows.reshape(length, heads, width)
    pieces = jnp.cumsum(jax.nn.log_sigmoid(forget_gate).reshape(heads, length // CUM, CUM), axis=-1)
    closing = pieces[..., -1]
    before = jnp.cumsum(closing, axis=-1) - closing
    cumulative = (pieces + before[..., None]).reshape(heads, length)
    decay = cumulative[:, -1]
    log_close = decay[:, None] - cumulative + in_gate
    level = jnp.max(log_close, axis=-1)
    close = jnp.exp(log_close - level[:, None]) * scale
    weighted = (k.astype(f32) * close.T[:, :, None]).astype(bf16)
    state = jnp.einsum("lhd,lhe->hde", weighted, v, preferred_element_type=f32)
    carried, carried_level = device_prefix(state, level, decay)

    causal = jnp.tril(jnp.ones((length, length), dtype=bool))
    log_inner = jnp.where(
        causal, cumulative[:, :, None] + (in_gate - cumulative)[:, None, :], -jnp.inf
    )
    log_inter = cumulative + carried_level[:, None]
    peak = jnp.maximum(log_inter, jnp.max(log_inner, axis=-1))
    scores = jnp.einsum("thd,shd->hts", q, k, preferred_element_type=f32) * scale
    scores = (scores * jnp.exp(log_inner - peak[..., None])).astype(bf16)
    from_block = jnp.einsum("hts,she->hte", scores, v, preferred_element_type=f32)
    from_state = jnp.einsum("thd,hde->hte", q, carried, preferred_element_type=f32)
    numerator = jnp.exp(log_inter - peak)[..., None] * from_state + from_block
    scaled = numerator * lax.rsqrt(
        jnp.mean(numerator * numerator, axis=-1, keepdims=True) + epsilon
    )
    gate = jax.nn.sigmoid(out_gate.astype(f32))
    return (scaled.transpose(1, 0, 2).reshape(length, heads * width) * gate).astype(bf16)


def slots_of(ids, first, capacity):
    rows, choices = ids.shape
    flat = ids.reshape(-1) - first
    onehot = (flat[:, None] == jnp.arange(GROUP)[None, :]).astype(bf16)
    count = rows * choices
    below = (jnp.arange(count)[:, None] > jnp.arange(count)[None, :]).astype(bf16)
    rank = jnp.sum(jnp.dot(below, onehot, preferred_element_type=f32) * onehot.astype(f32), axis=1)
    slot = flat * capacity + rank.astype(jnp.int32)
    inside = (flat >= 0) & (flat < GROUP)
    return jnp.where(inside, slot, -1).reshape(rows, choices)


def body(
    stream,
    queries,
    key_rows,
    value_rows,
    out_gate,
    in_gate,
    forget_gate,
    out_proj,
    ffn_gain,
    gate_proj,
    up_proj,
    down_proj,
    expert_ids,
    route_weights,
):
    total, mine = lax.axis_size("sp"), lax.axis_index("sp")
    groups = total // GROUP
    rows, width = stream.shape
    choices = expert_ids.shape[1]
    capacity = 2 * choices * rows // total
    cores = lax.axis_size("tp")

    def to_group(value, step):
        pairs = [
            (s, ((s // GROUP + step) % groups) * GROUP + s % GROUP) for s in range(total)
        ]
        return lax.ppermute(value, "sp", pairs)

    def other_core(value, step):
        return lax.ppermute(value, "tp", [(c, (c + step) % cores) for c in range(cores)])

    halves = [(gate_proj[0], up_proj[0], down_proj[0])] + [
        tuple(other_core(w[0], step) for w in (gate_proj, up_proj, down_proj))
        for step in range(1, cores)
    ]
    ids = [expert_ids] + [to_group(expert_ids, step) for step in range(1, groups)]
    shares = [route_weights] + [to_group(route_weights, step) for step in range(1, groups)]
    first = (mine // GROUP) * GROUP
    slot_count = GROUP * capacity
    places, backs = [], []
    for ids_one, share in zip(ids, shares):
        slot = slots_of(ids_one, first, capacity)
        hits = [
            (slot[:, j][None, :] == jnp.arange(slot_count)[:, None]) for j in range(choices)
        ]
        places.append(sum(hit.astype(bf16) for hit in hits))
        backs.append(sum(jnp.where(hits[j], share[:, j][None, :], 0.0) for j in range(choices)).astype(bf16))

    heads_out = mixer(queries, key_rows, value_rows, out_gate, in_gate, forget_gate)
    features = heads_out.shape[1]
    (token_heads,) = exchange(
        (heads_out.reshape(cores, rows, features),), ("slab",), "tp", cores, 3, 2_000_000
    )
    mix = sum(
        jnp.dot(token_heads[c], out_proj[c * features : (c + 1) * features], preferred_element_type=f32)
        for c in range(cores)
    )
    middle = (stream.astype(f32) + mix).astype(bf16)
    middle_float = middle.astype(f32)
    normed = (
        middle_float
        * lax.rsqrt(jnp.mean(middle_float * middle_float, axis=-1, keepdims=True) + epsilon)
        * ffn_gain
    ).astype(bf16)

    def experts(arrived):
        out = 0.0
        for gate, up, down in halves:
            hidden = (
                jax.nn.silu(jnp.dot(arrived, gate, preferred_element_type=f32))
                * jnp.dot(arrived, up, preferred_element_type=f32)
            ).astype(bf16)
            out = out + jnp.dot(hidden, down, preferred_element_type=f32)
        return out.astype(bf16)

    def round_trip(token_rows, place, back, turn):
        sent = jnp.dot(place, token_rows, preferred_element_type=f32).astype(bf16)
        cost = 40_000_000
        (arrived,) = exchange(
            (sent.reshape(GROUP, capacity, width),), ("slab",), "sp", GROUP, 4 + 2 * turn, cost
        )
        result = experts(arrived.reshape(slot_count, width)).reshape(GROUP, capacity, width)
        (returned,) = exchange((result,), ("slab",), "sp", GROUP, 5 + 2 * turn, cost)
        return lax.dot_general(
            back,
            returned.reshape(slot_count, width),
            (((0,), (0,)), ((), ())),
            preferred_element_type=f32,
        )

    crossing = [to_group(normed, step) for step in range(1, groups)]
    own = round_trip(normed, places[0], backs[0], 0)
    expert_sum = own
    for step in range(1, groups):
        done = round_trip(crossing[step - 1], places[step], backs[step], step).astype(bf16)
        expert_sum = expert_sum + to_group(done, groups - step).astype(f32)
    return (middle_float + expert_sum).astype(bf16)


def solution(mesh):
    in_specs = (
        P(("sp", "tp"), None),
        P("sp", "tp"),
        P("sp", "tp"),
        P("sp", "tp"),
        P("sp", "tp"),
        P("tp", "sp"),
        P("tp", "sp"),
        P(),
        P(),
        P("sp", None, "tp"),
        P("sp", None, "tp"),
        P("sp", "tp", None),
        P(("sp", "tp"), None),
        P(("sp", "tp"), None),
    )
    out_specs = P(("sp", "tp"), None)
    return jax.shard_map(body, mesh=mesh, in_specs=in_specs, out_specs=out_specs, check_vma=False)
```

```python
import functools

import jax
import jax.numpy as jnp
from jax import lax
from jax.experimental import pallas as pl
from jax.experimental.pallas import tpu as pltpu
from jax.sharding import PartitionSpec as P

GROUP = 8
CUM = 64
epsilon = 1e-06
bf16, f32 = jnp.bfloat16, jnp.float32


def exchange_kernel(axis, group, count, kinds, *refs):
    ins, outs = refs[:count], refs[count : 2 * count]
    send, recv = refs[2 * count :]
    mine = lax.axis_index(axis)
    base = (mine // group) * group
    me = mine - base

    barrier = pltpu.get_barrier_semaphore()
    for step in range(1, group):
        peer = base + lax.rem(me + step, group)
        pl.semaphore_signal(barrier, inc=1, device_id={axis: peer}, device_id_type=pl.DeviceIdType.MESH)
    pl.semaphore_wait(barrier, group - 1)
    copies = []
    for step in range(1, group):
        to = lax.rem(me + step, group)
        for n in range(count):
            copy = pltpu.make_async_remote_copy(
                src_ref=ins[n].at[to] if kinds[n] == "slab" else ins[n],
                dst_ref=outs[n].at[me],
                send_sem=send.at[n, step],
                recv_sem=recv.at[n, step],
                device_id={axis: base + to},
                device_id_type=pl.DeviceIdType.MESH,
            )
            copy.start()
            copies.append(copy)
    for n in range(count):
        outs[n][me] = ins[n][me] if kinds[n] == "slab" else ins[n][...]
    for copy in copies:
        copy.wait()


def exchange(arrays, kinds, axis, group, collective_id, cost):
    count = len(arrays)
    out_shape = [
        jax.ShapeDtypeStruct(a.shape if kind == "slab" else (group,) + a.shape, a.dtype)
        for a, kind in zip(arrays, kinds)
    ]
    return pl.pallas_call(
        functools.partial(exchange_kernel, axis, group, count, kinds),
        out_shape=out_shape,
        in_specs=[pl.BlockSpec(memory_space=pltpu.VMEM)] * count,
        out_specs=[pl.BlockSpec(memory_space=pltpu.VMEM)] * count,
        scratch_shapes=[
            pltpu.SemaphoreType.DMA((count, group)),
            pltpu.SemaphoreType.DMA((count, group)),
        ],
        compiler_params=pltpu.CompilerParams(collective_id=collective_id, has_side_effects=True),
        cost_estimate=pl.CostEstimate(flops=0, bytes_accessed=cost, transcendentals=0),
    )(*arrays)


def device_prefix(state, level, decay):
    total, mine = lax.axis_size("sp"), lax.axis_index("sp")
    heads, qk, width = state.shape
    rows = heads * qk // total
    slabs = state.astype(bf16).reshape(total, rows, width)
    info = jnp.zeros((8, 128), f32).at[0, :heads].set(level).at[1, :heads].set(decay)
    slabs, infos = exchange((slabs, info), ("slab", "all"), "sp", total, 1, 10_000_000)
    levels, decays = infos[:, 0, :heads].T, infos[:, 1, :heads].T
    order = jnp.arange(total)
    between = (order[None, :, None] < order[None, None, :]) & (order[None, None, :] < order[:, None, None])
    gap = jnp.sum(jnp.where(between[None], decays[:, None, None, :], 0.0), axis=-1)
    earlier = order[None, :] < order[:, None]
    reach = jnp.where(earlier[None], levels[:, None, :] + gap, -jnp.inf)
    start = jnp.sum(jnp.where(earlier[None], decays[:, None, :], 0.0), axis=-1)
    top = jnp.maximum(start, jnp.max(reach, axis=-1))
    weights = jnp.exp(reach - top[..., None])
    head_here = mine * heads // total
    weight = lax.dynamic_index_in_dim(weights, head_here, 0, keepdims=False)
    prefix = jnp.dot(
        weight, slabs.astype(f32).reshape(total, rows * width), precision=lax.Precision.HIGHEST
    )
    prefix = prefix.astype(bf16).reshape(total, rows, width)
    (prefix,) = exchange((prefix,), ("slab",), "sp", total, 2, 10_000_000)
    top_mine = lax.dynamic_index_in_dim(top, mine, 1, keepdims=False)
    return prefix.reshape(heads, qk, width), top_mine


def mixer(queries, key_rows, value_rows, out_gate, in_gate, forget_gate):
    heads, length = in_gate.shape
    qk, width = queries.shape[1] // heads, value_rows.shape[1] // heads
    scale = qk ** (-0.5)
    q = queries.reshape(length, heads, qk)
    k = key_rows.reshape(length, heads, qk)
    v = value_rows.reshape(length, heads, width)
    pieces = jnp.cumsum(jax.nn.log_sigmoid(forget_gate).reshape(heads, length // CUM, CUM), axis=-1)
    closing = pieces[..., -1]
    before = jnp.cumsum(closing, axis=-1) - closing
    cumulative = (pieces + before[..., None]).reshape(heads, length)
    decay = cumulative[:, -1]
    log_close = decay[:, None] - cumulative + in_gate
    level = jnp.max(log_close, axis=-1)
    close = jnp.exp(log_close - level[:, None]) * scale
    weighted = (k.astype(f32) * close.T[:, :, None]).astype(bf16)
    state = jnp.einsum("lhd,lhe->hde", weighted, v, preferred_element_type=f32)
    carried, carried_level = device_prefix(state, level, decay)

    causal = jnp.tril(jnp.ones((length, length), dtype=bool))
    log_inner = jnp.where(
        causal, cumulative[:, :, None] + (in_gate - cumulative)[:, None, :], -jnp.inf
    )
    log_inter = cumulative + carried_level[:, None]
    peak = jnp.maximum(log_inter, jnp.max(log_inner, axis=-1))
    scores = jnp.einsum("thd,shd->hts", q, k, preferred_element_type=f32) * scale
    scores = (scores * jnp.exp(log_inner - peak[..., None])).astype(bf16)
    from_block = jnp.einsum("hts,she->hte", scores, v, preferred_element_type=f32)
    from_state = jnp.einsum("thd,hde->hte", q, carried, preferred_element_type=f32)
    numerator = jnp.exp(log_inter - peak)[..., None] * from_state + from_block
    scaled = numerator * lax.rsqrt(
        jnp.mean(numerator * numerator, axis=-1, keepdims=True) + epsilon
    )
    gate = jax.nn.sigmoid(out_gate.astype(f32))
    return (scaled.transpose(1, 0, 2).reshape(length, heads * width) * gate).astype(bf16)


def slots_of(ids, first, capacity):
    rows, choices = ids.shape
    flat = ids.reshape(-1) - first
    onehot = (flat[:, None] == jnp.arange(GROUP)[None, :]).astype(bf16)
    count = rows * choices
    below = (jnp.arange(count)[:, None] > jnp.arange(count)[None, :]).astype(bf16)
    rank = jnp.sum(jnp.dot(below, onehot, preferred_element_type=f32) * onehot.astype(f32), axis=1)
    slot = flat * capacity + rank.astype(jnp.int32)
    inside = (flat >= 0) & (flat < GROUP)
    return jnp.where(inside, slot, -1).reshape(rows, choices)


CHUNKS = 2
TILE = 256
FLIPS = (7, 3, 5, 6, 1, 2, 4)


def flip(member, bits):
    for power in (1, 2, 4):
        if bits & power:
            member = member + power * (1 - 2 * (lax.rem(lax.div(member, power), 2)))
    return member


def expert_kernel(groups, capacity, halves, *refs):
    normed, middle, places, backs = refs[:4]
    weights_hbm = refs[4 : 4 + 3 * halves]
    out = refs[4 + 3 * halves]
    rest = refs[5 + 3 * halves :]
    weights = rest[: 3 * halves]
    crossed, combined, crossed_back, own_sum, hidden = rest[3 * halves : 3 * halves + 5]
    sent0, arrived0, result0, back0, sent1, arrived1, result1, back1 = rest[
        3 * halves + 5 : 3 * halves + 13
    ]
    load_sem, cross_s, cross_r, home_s, home_r, own_s, own_r, oth_s, oth_r = rest[3 * halves + 13 :]
    rows, width = normed.shape
    part = width // CHUNKS
    extra = groups - 1
    mine = lax.axis_index("sp")
    group = lax.div(mine, GROUP)
    base = group * GROUP
    me = mine - base
    far = lambda step: lax.rem(group + step, groups) * GROUP + me

    loads = [
        pltpu.make_async_copy(src, dst, load_sem.at[n])
        for n, (src, dst) in enumerate(zip(weights_hbm, weights))
    ]
    for load in loads:
        load.start()
    barrier = pltpu.get_barrier_semaphore()
    peers = [base + flip(me, bits) for bits in FLIPS] + [far(step) for step in range(1, groups)]
    for peer in peers:
        pl.semaphore_signal(
            barrier, inc=1, device_id={"sp": peer}, device_id_type=pl.DeviceIdType.MESH
        )
    pl.semaphore_wait(barrier, len(peers))

    def send(src, dst, send_sem, recv_sem, peer):
        copy = pltpu.make_async_remote_copy(
            src_ref=src,
            dst_ref=dst,
            send_sem=send_sem,
            recv_sem=recv_sem,
            device_id={"sp": peer},
            device_id_type=pl.DeviceIdType.MESH,
        )
        copy.start()
        return copy

    def box_send(src, dst, send_sem, recv_sem, cols):
        copies = []
        for n, bits in enumerate(FLIPS):
            to = flip(me, bits)
            copies.append(
                send(
                    src.at[to, :, cols],
                    dst.at[me, :, cols],
                    send_sem.at[n],
                    recv_sem.at[n],
                    base + to,
                )
            )
        return copies

    def tiles(start, stop, body):
        def turn(n, carry):
            body(pl.ds(pl.multiple_of(start + n * TILE, TILE), TILE))
            return carry

        lax.fori_loop(0, (stop - start) // TILE, turn, 0)

    def columns(chunk):
        return pl.ds(chunk * part, part)

    crossing = [
        [
            send(
                normed.at[:, columns(chunk)],
                crossed.at[step - 1, :, columns(chunk)],
                cross_s.at[step - 1, chunk],
                cross_r.at[step - 1, chunk],
                far(step),
            )
            for step in range(1, groups)
        ]
        for chunk in range(CHUNKS)
    ]

    def place_own(cols):
        value = jnp.dot(places[0], normed[:, cols], preferred_element_type=f32)
        sent0[:, :, cols] = value.astype(bf16).reshape(GROUP, capacity, TILE)

    tiles(0, width, place_own)
    own = box_send(sent0, arrived0, own_s.at[0], own_r.at[0], pl.ds(0, width))
    arrived0[me] = sent0[me]

    others = []
    for chunk in range(CHUNKS):
        for copy in crossing[chunk]:
            copy.wait()

        def place_other(cols):
            for step in range(extra):
                value = jnp.dot(
                    places[step + 1], crossed[step, :, cols], preferred_element_type=f32
                )
                sent1[:, step * capacity : (step + 1) * capacity, cols] = value.astype(
                    bf16
                ).reshape(GROUP, capacity, TILE)

        tiles(chunk * part, (chunk + 1) * part, place_other)
        others += box_send(sent1, arrived1, oth_s.at[chunk], oth_r.at[chunk], columns(chunk))
    arrived1[me] = sent1[me]

    def make_hidden(arrived, amount):
        wide = GROUP * amount
        members = max(1, min(GROUP, TILE // amount))
        high = members * amount

        def turn(n, carry):
            value = arrived[pl.ds(n * members, members)].reshape(high, width)
            for half in range(halves):
                gate = jnp.dot(value, weights[3 * half][...], preferred_element_type=f32)
                up = jnp.dot(value, weights[3 * half + 1][...], preferred_element_type=f32)
                units = gate.shape[1]
                hidden[pl.ds(pl.multiple_of(n * high, 16), high), half * units : (half + 1) * units] = (
                    gate * jax.nn.sigmoid(gate) * up
                ).astype(bf16)
            return carry

        lax.fori_loop(0, wide // high, turn, 0)

    def make_result(result, amount, chunk, parts):
        wide = GROUP * amount
        units = weights[2].shape[0]
        step = width // parts

        def one(cols):
            value = sum(
                jnp.dot(
                    hidden[:wide, half * units : (half + 1) * units],
                    weights[3 * half + 2][:, cols],
                    preferred_element_type=f32,
                )
                for half in range(halves)
            )
            result[:, :, cols] = value.astype(bf16).reshape(GROUP, amount, TILE)

        tiles(chunk * step, (chunk + 1) * step, one)

    for load in loads:
        load.wait()
    for copy in own:
        copy.wait()
    make_hidden(arrived0, capacity)
    make_result(result0, capacity, 0, 1)

    for copy in others:
        copy.wait()
    returns = []
    if extra:
        make_hidden(arrived1, extra * capacity)
        for chunk in range(CHUNKS):
            make_result(result1, extra * capacity, chunk, CHUNKS)
            at = CHUNKS + chunk
            returns.append(box_send(result1, back1, oth_s.at[at], oth_r.at[at], columns(chunk)))
        back1[me] = result1[me]
    own_return = box_send(result0, back0, own_s.at[1], own_r.at[1], pl.ds(0, width))
    back0[me] = result0[me]

    homeward = []
    for chunk in range(CHUNKS):
        for copy in returns[chunk]:
            copy.wait()

        def combine(cols):
            for step in range(extra):
                value = back1[:, step * capacity : (step + 1) * capacity, cols]
                combined[step, :, cols] = jnp.dot(
                    backs[step + 1],
                    value.reshape(GROUP * capacity, TILE),
                    preferred_element_type=f32,
                ).astype(bf16)

        tiles(chunk * part, (chunk + 1) * part, combine)
        homeward.append(
            [
                send(
                    combined.at[step, :, columns(chunk)],
                    crossed_back.at[step, :, columns(chunk)],
                    home_s.at[step, chunk],
                    home_r.at[step, chunk],
                    far(groups - 1 - step),
                )
                for step in range(extra)
            ]
        )

    for copy in own_return:
        copy.wait()

    def combine_own(cols):
        own_sum[:, cols] = middle[:, cols].astype(f32) + jnp.dot(
            backs[0],
            back0[:, :, cols].reshape(GROUP * capacity, TILE),
            preferred_element_type=f32,
        )

    tiles(0, width, combine_own)
    for chunk in range(CHUNKS):
        for copy in homeward[chunk]:
            copy.wait()
        cols = slice(chunk * part, (chunk + 1) * part)
        total = own_sum[:, cols]
        for step in range(extra):
            total = total + crossed_back[step, :, cols].astype(f32)
        out[:, cols] = total.astype(bf16)


def expert_layer(arrays, weights, groups, capacity):
    rows, width = arrays[0].shape
    extra = groups - 1
    halves = len(weights) // 3
    units = sum(weights[3 * half].shape[1] for half in range(halves))
    own = pltpu.VMEM((GROUP, capacity, width), bf16)
    other = pltpu.VMEM((GROUP, extra * capacity, width), bf16)
    cross = pltpu.VMEM((extra, rows, width), bf16)
    dma = pltpu.SemaphoreType.DMA
    scratch = [pltpu.VMEM(w.shape, w.dtype) for w in weights]
    scratch += [cross, cross, cross, pltpu.VMEM((rows, width), f32)]
    scratch += [pltpu.VMEM((GROUP * max(1, extra) * capacity, units), bf16)]
    scratch += [own] * 4 + [other] * 4
    scratch += [dma((len(weights),))] + [dma((extra, CHUNKS))] * 4
    scratch += [dma((2, len(FLIPS)))] * 2 + [dma((2 * CHUNKS, len(FLIPS)))] * 2
    vmem, anywhere = pl.BlockSpec(memory_space=pltpu.VMEM), pl.BlockSpec(memory_space=pl.ANY)
    return pl.pallas_call(
        functools.partial(expert_kernel, groups, capacity, halves),
        out_shape=jax.ShapeDtypeStruct((rows, width), bf16),
        in_specs=[vmem] * 4 + [anywhere] * len(weights),
        out_specs=vmem,
        scratch_shapes=scratch,
        compiler_params=pltpu.CompilerParams(
            collective_id=4, has_side_effects=True, vmem_limit_bytes=64 * 1024 * 1024 - 65536
        ),
        cost_estimate=pl.CostEstimate(
            flops=10_000_000_000, bytes_accessed=100_000_000, transcendentals=0
        ),
    )(*arrays, *weights)


def body(
    stream,
    queries,
    key_rows,
    value_rows,
    out_gate,
    in_gate,
    forget_gate,
    out_proj,
    ffn_gain,
    gate_proj,
    up_proj,
    down_proj,
    expert_ids,
    route_weights,
):
    total, mine = lax.axis_size("sp"), lax.axis_index("sp")
    groups = total // GROUP
    rows, width = stream.shape
    choices = expert_ids.shape[1]
    capacity = 2 * choices * rows // total
    cores = lax.axis_size("tp")

    def to_group(value, step):
        pairs = [
            (s, ((s // GROUP + step) % groups) * GROUP + s % GROUP) for s in range(total)
        ]
        return lax.ppermute(value, "sp", pairs)

    def other_core(value, step):
        return lax.ppermute(value, "tp", [(c, (c + step) % cores) for c in range(cores)])

    halves = [(gate_proj[0], up_proj[0], down_proj[0])] + [
        tuple(other_core(w[0], step) for w in (gate_proj, up_proj, down_proj))
        for step in range(1, cores)
    ]
    ids = [expert_ids] + [to_group(expert_ids, step) for step in range(1, groups)]
    shares = [route_weights] + [to_group(route_weights, step) for step in range(1, groups)]
    first = (mine // GROUP) * GROUP
    slot_count = GROUP * capacity
    places, backs = [], []
    for ids_one, share in zip(ids, shares):
        slot = slots_of(ids_one, first, capacity)
        here = jnp.arange(slot_count)
        places.append(
            sum((slot[:, j][None, :] == here[:, None]).astype(bf16) for j in range(choices))
        )
        backs.append(
            sum(
                jnp.where(slot[:, j][:, None] == here[None, :], share[:, j][:, None], 0.0)
                for j in range(choices)
            ).astype(bf16)
        )

    heads_out = mixer(queries, key_rows, value_rows, out_gate, in_gate, forget_gate)
    features = heads_out.shape[1]
    (token_heads,) = exchange(
        (heads_out.reshape(cores, rows, features),), ("slab",), "tp", cores, 3, 2_000_000
    )
    mix = sum(
        jnp.dot(token_heads[c], out_proj[c * features : (c + 1) * features], preferred_element_type=f32)
        for c in range(cores)
    )
    middle = (stream.astype(f32) + mix).astype(bf16)
    middle_float = middle.astype(f32)
    normed = (
        middle_float
        * lax.rsqrt(jnp.mean(middle_float * middle_float, axis=-1, keepdims=True) + epsilon)
        * ffn_gain
    ).astype(bf16)

    arrays = (normed, middle, jnp.stack(places), jnp.stack(backs))
    return expert_layer(arrays, [w for half in halves for w in half], groups, capacity)


def solution(mesh):
    in_specs = (
        P(("sp", "tp"), None),
        P("sp", "tp"),
        P("sp", "tp"),
        P("sp", "tp"),
        P("sp", "tp"),
        P("tp", "sp"),
        P("tp", "sp"),
        P(),
        P(),
        P("sp", None, "tp"),
        P("sp", None, "tp"),
        P("sp", "tp", None),
        P(("sp", "tp"), None),
        P(("sp", "tp"), None),
    )
    out_specs = P(("sp", "tp"), None)
    return jax.shard_map(body, mesh=mesh, in_specs=in_specs, out_specs=out_specs, check_vma=False)
```

```python
import functools

import jax
import jax.numpy as jnp
from jax import lax
from jax.experimental import pallas as pl
from jax.experimental.pallas import tpu as pltpu
from jax.sharding import PartitionSpec as P

GROUP = 8
CUM = 64
epsilon = 1e-06
bf16, f32 = jnp.bfloat16, jnp.float32


def exchange_kernel(axis, group, count, kinds, *refs):
    ins, outs = refs[:count], refs[count : 2 * count]
    send, recv = refs[2 * count :]
    mine = lax.axis_index(axis)
    base = (mine // group) * group
    me = mine - base

    barrier = pltpu.get_barrier_semaphore()
    for step in range(1, group):
        peer = base + lax.rem(me + step, group)
        pl.semaphore_signal(barrier, inc=1, device_id={axis: peer}, device_id_type=pl.DeviceIdType.MESH)
    pl.semaphore_wait(barrier, group - 1)
    copies = []
    for step in range(1, group):
        to = lax.rem(me + step, group)
        for n in range(count):
            copy = pltpu.make_async_remote_copy(
                src_ref=ins[n].at[to] if kinds[n] == "slab" else ins[n],
                dst_ref=outs[n].at[me],
                send_sem=send.at[n, step],
                recv_sem=recv.at[n, step],
                device_id={axis: base + to},
                device_id_type=pl.DeviceIdType.MESH,
            )
            copy.start()
            copies.append(copy)
    for n in range(count):
        outs[n][me] = ins[n][me] if kinds[n] == "slab" else ins[n][...]
    for copy in copies:
        copy.wait()


def exchange(arrays, kinds, axis, group, collective_id, cost):
    count = len(arrays)
    out_shape = [
        jax.ShapeDtypeStruct(a.shape if kind == "slab" else (group,) + a.shape, a.dtype)
        for a, kind in zip(arrays, kinds)
    ]
    return pl.pallas_call(
        functools.partial(exchange_kernel, axis, group, count, kinds),
        out_shape=out_shape,
        in_specs=[pl.BlockSpec(memory_space=pltpu.VMEM)] * count,
        out_specs=[pl.BlockSpec(memory_space=pltpu.VMEM)] * count,
        scratch_shapes=[
            pltpu.SemaphoreType.DMA((count, group)),
            pltpu.SemaphoreType.DMA((count, group)),
        ],
        compiler_params=pltpu.CompilerParams(collective_id=collective_id, has_side_effects=True),
        cost_estimate=pl.CostEstimate(flops=0, bytes_accessed=cost, transcendentals=0),
    )(*arrays)


def device_prefix(state, level, decay):
    total, mine = lax.axis_size("sp"), lax.axis_index("sp")
    heads, qk, width = state.shape
    rows = heads * qk // total
    slabs = state.astype(bf16).reshape(total, rows, width)
    info = jnp.zeros((8, 128), f32).at[0, :heads].set(level).at[1, :heads].set(decay)
    slabs, infos = exchange((slabs, info), ("slab", "all"), "sp", total, 1, 10_000_000)
    levels, decays = infos[:, 0, :heads].T, infos[:, 1, :heads].T
    order = jnp.arange(total)
    between = (order[None, :, None] < order[None, None, :]) & (order[None, None, :] < order[:, None, None])
    gap = jnp.sum(jnp.where(between[None], decays[:, None, None, :], 0.0), axis=-1)
    earlier = order[None, :] < order[:, None]
    reach = jnp.where(earlier[None], levels[:, None, :] + gap, -jnp.inf)
    start = jnp.sum(jnp.where(earlier[None], decays[:, None, :], 0.0), axis=-1)
    top = jnp.maximum(start, jnp.max(reach, axis=-1))
    weights = jnp.exp(reach - top[..., None])
    head_here = mine * heads // total
    weight = lax.dynamic_index_in_dim(weights, head_here, 0, keepdims=False)
    prefix = jnp.dot(
        weight, slabs.astype(f32).reshape(total, rows * width), precision=lax.Precision.HIGHEST
    )
    prefix = prefix.astype(bf16).reshape(total, rows, width)
    (prefix,) = exchange((prefix,), ("slab",), "sp", total, 2, 10_000_000)
    top_mine = lax.dynamic_index_in_dim(top, mine, 1, keepdims=False)
    return prefix.reshape(heads, qk, width), top_mine


def mixer(queries, key_rows, value_rows, out_gate, in_gate, forget_gate):
    heads, length = in_gate.shape
    qk, width = queries.shape[1] // heads, value_rows.shape[1] // heads
    scale = qk ** (-0.5)
    q = queries.reshape(length, heads, qk)
    k = key_rows.reshape(length, heads, qk)
    v = value_rows.reshape(length, heads, width)
    pieces = jnp.cumsum(jax.nn.log_sigmoid(forget_gate).reshape(heads, length // CUM, CUM), axis=-1)
    closing = pieces[..., -1]
    before = jnp.cumsum(closing, axis=-1) - closing
    cumulative = (pieces + before[..., None]).reshape(heads, length)
    decay = cumulative[:, -1]
    log_close = decay[:, None] - cumulative + in_gate
    level = jnp.max(log_close, axis=-1)
    close = jnp.exp(log_close - level[:, None]) * scale
    weighted = (k.astype(f32) * close.T[:, :, None]).astype(bf16)
    state = jnp.einsum("lhd,lhe->hde", weighted, v, preferred_element_type=f32)
    carried, carried_level = device_prefix(state, level, decay)

    causal = jnp.tril(jnp.ones((length, length), dtype=bool))
    log_inner = jnp.where(
        causal, cumulative[:, :, None] + (in_gate - cumulative)[:, None, :], -jnp.inf
    )
    log_inter = cumulative + carried_level[:, None]
    peak = jnp.maximum(log_inter, jnp.max(log_inner, axis=-1))
    scores = jnp.einsum("thd,shd->hts", q, k, preferred_element_type=f32) * scale
    scores = (scores * jnp.exp(log_inner - peak[..., None])).astype(bf16)
    from_block = jnp.einsum("hts,she->hte", scores, v, preferred_element_type=f32)
    from_state = jnp.einsum("thd,hde->hte", q, carried, preferred_element_type=f32)
    numerator = jnp.exp(log_inter - peak)[..., None] * from_state + from_block
    scaled = numerator * lax.rsqrt(
        jnp.mean(numerator * numerator, axis=-1, keepdims=True) + epsilon
    )
    gate = jax.nn.sigmoid(out_gate.astype(f32))
    return (scaled.transpose(1, 0, 2).reshape(length, heads * width) * gate).astype(bf16)


def slots_of(ids, first, capacity):
    rows, choices = ids.shape
    flat = ids.reshape(-1) - first
    onehot = (flat[:, None] == jnp.arange(GROUP)[None, :]).astype(bf16)
    count = rows * choices
    below = (jnp.arange(count)[:, None] > jnp.arange(count)[None, :]).astype(bf16)
    rank = jnp.sum(jnp.dot(below, onehot, preferred_element_type=f32) * onehot.astype(f32), axis=1)
    slot = flat * capacity + rank.astype(jnp.int32)
    inside = (flat >= 0) & (flat < GROUP)
    return jnp.where(inside, slot, -1).reshape(rows, choices)


CHUNKS = 4
TILE = 256
FLIPS = (7, 3, 5, 6, 1, 2, 4)
ACROSS = 4


def flip(member, bits):
    for power in (1, 2, 4):
        if bits & power:
            member = member + power * (1 - 2 * (lax.rem(lax.div(member, power), 2)))
    return member


def expert_kernel(groups, capacity, halves, *refs):
    normed, middle, places, backs = refs[:4]
    weights_hbm = refs[4 : 4 + 3 * halves]
    out = refs[4 + 3 * halves]
    rest = refs[5 + 3 * halves :]
    weights = rest[: 3 * halves]
    crossed, combined, crossed_back, own_sum, hidden = rest[3 * halves : 3 * halves + 5]
    sent0, arrived0, result0, back0, sent1, arrived1, result1, back1 = rest[
        3 * halves + 5 : 3 * halves + 13
    ]
    load_sem, cross_s, cross_r, home_s, home_r, own_s, own_r, oth_s, oth_r = rest[3 * halves + 13 :]
    rows, width = normed.shape
    part = width // CHUNKS
    extra = groups - 1
    mine = lax.axis_index("sp")
    group = lax.div(mine, GROUP)
    base = group * GROUP
    me = mine - base
    far = lambda step: lax.rem(group + step, groups) * GROUP + flip(me, ACROSS)

    loads = [
        pltpu.make_async_copy(src, dst, load_sem.at[n])
        for n, (src, dst) in enumerate(zip(weights_hbm, weights))
    ]
    for load in loads:
        load.start()
    barrier = pltpu.get_barrier_semaphore()
    peers = [base + flip(me, bits) for bits in FLIPS] + [far(step) for step in range(1, groups)]
    for peer in peers:
        pl.semaphore_signal(
            barrier, inc=1, device_id={"sp": peer}, device_id_type=pl.DeviceIdType.MESH
        )
    pl.semaphore_wait(barrier, len(peers))

    def send(src, dst, send_sem, recv_sem, peer):
        copy = pltpu.make_async_remote_copy(
            src_ref=src,
            dst_ref=dst,
            send_sem=send_sem,
            recv_sem=recv_sem,
            device_id={"sp": peer},
            device_id_type=pl.DeviceIdType.MESH,
        )
        copy.start()
        return copy

    def box_send(src, dst, send_sem, recv_sem, cols):
        copies = []
        for n, bits in enumerate(FLIPS):
            to = flip(me, bits)
            copies.append(
                send(
                    src.at[to, :, cols],
                    dst.at[me, :, cols],
                    send_sem.at[n],
                    recv_sem.at[n],
                    base + to,
                )
            )
        return copies

    def tiles(start, stop, body):
        def turn(n, carry):
            body(pl.ds(pl.multiple_of(start + n * TILE, TILE), TILE))
            return carry

        lax.fori_loop(0, (stop - start) // TILE, turn, 0)

    def columns(chunk):
        return pl.ds(chunk * part, part)

    crossing = [
        [
            send(
                normed.at[:, columns(chunk)],
                crossed.at[step - 1, :, columns(chunk)],
                cross_s.at[step - 1, chunk],
                cross_r.at[step - 1, chunk],
                far(step),
            )
            for step in range(1, groups)
        ]
        for chunk in range(CHUNKS)
    ]

    def place_own(cols):
        value = jnp.dot(places[0], normed[:, cols], preferred_element_type=f32)
        sent0[:, :, cols] = value.astype(bf16).reshape(GROUP, capacity, TILE)

    tiles(0, width, place_own)
    own = box_send(sent0, arrived0, own_s.at[0], own_r.at[0], pl.ds(0, width))
    arrived0[me] = sent0[me]

    others = []
    for chunk in range(CHUNKS):
        for copy in crossing[chunk]:
            copy.wait()

        def place_other(cols):
            for step in range(extra):
                value = jnp.dot(
                    places[step + 1], crossed[step, :, cols], preferred_element_type=f32
                )
                sent1[:, step * capacity : (step + 1) * capacity, cols] = value.astype(
                    bf16
                ).reshape(GROUP, capacity, TILE)

        tiles(chunk * part, (chunk + 1) * part, place_other)
        others += box_send(sent1, arrived1, oth_s.at[chunk], oth_r.at[chunk], columns(chunk))
    arrived1[me] = sent1[me]

    def make_hidden(arrived, amount):
        wide = GROUP * amount
        members = max(1, min(GROUP, TILE // amount))
        high = members * amount

        def turn(n, carry):
            value = arrived[pl.ds(n * members, members)].reshape(high, width)
            for half in range(halves):
                gate = jnp.dot(value, weights[3 * half][...], preferred_element_type=f32)
                up = jnp.dot(value, weights[3 * half + 1][...], preferred_element_type=f32)
                units = gate.shape[1]
                hidden[pl.ds(pl.multiple_of(n * high, 16), high), half * units : (half + 1) * units] = (
                    gate * jax.nn.sigmoid(gate) * up
                ).astype(bf16)
            return carry

        lax.fori_loop(0, wide // high, turn, 0)

    def make_result(result, amount, chunk, parts):
        wide = GROUP * amount
        units = weights[2].shape[0]
        step = width // parts

        def one(cols):
            value = sum(
                jnp.dot(
                    hidden[:wide, half * units : (half + 1) * units],
                    weights[3 * half + 2][:, cols],
                    preferred_element_type=f32,
                )
                for half in range(halves)
            )
            result[:, :, cols] = value.astype(bf16).reshape(GROUP, amount, TILE)

        tiles(chunk * step, (chunk + 1) * step, one)

    for load in loads:
        load.wait()
    for copy in own:
        copy.wait()
    make_hidden(arrived0, capacity)
    make_result(result0, capacity, 0, 1)

    for copy in others:
        copy.wait()
    returns = []
    if extra:
        make_hidden(arrived1, extra * capacity)
        for chunk in range(CHUNKS):
            make_result(result1, extra * capacity, chunk, CHUNKS)
            at = CHUNKS + chunk
            returns.append(box_send(result1, back1, oth_s.at[at], oth_r.at[at], columns(chunk)))
        back1[me] = result1[me]
    own_return = box_send(result0, back0, own_s.at[1], own_r.at[1], pl.ds(0, width))
    back0[me] = result0[me]

    homeward = []
    for chunk in range(CHUNKS):
        for copy in returns[chunk]:
            copy.wait()

        def combine(cols):
            for step in range(extra):
                value = back1[:, step * capacity : (step + 1) * capacity, cols]
                combined[step, :, cols] = jnp.dot(
                    backs[step + 1],
                    value.reshape(GROUP * capacity, TILE),
                    preferred_element_type=f32,
                ).astype(bf16)

        tiles(chunk * part, (chunk + 1) * part, combine)
        homeward.append(
            [
                send(
                    combined.at[step, :, columns(chunk)],
                    crossed_back.at[step, :, columns(chunk)],
                    home_s.at[step, chunk],
                    home_r.at[step, chunk],
                    far(groups - 1 - step),
                )
                for step in range(extra)
            ]
        )

    for copy in own_return:
        copy.wait()

    def combine_own(cols):
        own_sum[:, cols] = middle[:, cols].astype(f32) + jnp.dot(
            backs[0],
            back0[:, :, cols].reshape(GROUP * capacity, TILE),
            preferred_element_type=f32,
        )

    tiles(0, width, combine_own)
    for chunk in range(CHUNKS):
        for copy in homeward[chunk]:
            copy.wait()
        cols = slice(chunk * part, (chunk + 1) * part)
        total = own_sum[:, cols]
        for step in range(extra):
            total = total + crossed_back[step, :, cols].astype(f32)
        out[:, cols] = total.astype(bf16)


def expert_layer(arrays, weights, groups, capacity):
    rows, width = arrays[0].shape
    extra = groups - 1
    halves = len(weights) // 3
    units = sum(weights[3 * half].shape[1] for half in range(halves))
    own = pltpu.VMEM((GROUP, capacity, width), bf16)
    other = pltpu.VMEM((GROUP, extra * capacity, width), bf16)
    cross = pltpu.VMEM((extra, rows, width), bf16)
    dma = pltpu.SemaphoreType.DMA
    scratch = [pltpu.VMEM(w.shape, w.dtype) for w in weights]
    scratch += [cross, cross, cross, pltpu.VMEM((rows, width), f32)]
    scratch += [pltpu.VMEM((GROUP * max(1, extra) * capacity, units), bf16)]
    scratch += [own] * 4 + [other] * 4
    scratch += [dma((len(weights),))] + [dma((extra, CHUNKS))] * 4
    scratch += [dma((2, len(FLIPS)))] * 2 + [dma((2 * CHUNKS, len(FLIPS)))] * 2
    vmem, anywhere = pl.BlockSpec(memory_space=pltpu.VMEM), pl.BlockSpec(memory_space=pl.ANY)
    return pl.pallas_call(
        functools.partial(expert_kernel, groups, capacity, halves),
        out_shape=jax.ShapeDtypeStruct((rows, width), bf16),
        in_specs=[vmem] * 4 + [anywhere] * len(weights),
        out_specs=vmem,
        scratch_shapes=scratch,
        compiler_params=pltpu.CompilerParams(
            collective_id=4, has_side_effects=True, vmem_limit_bytes=64 * 1024 * 1024 - 65536
        ),
        cost_estimate=pl.CostEstimate(
            flops=10_000_000_000, bytes_accessed=100_000_000, transcendentals=0
        ),
    )(*arrays, *weights)


def body(
    stream,
    queries,
    key_rows,
    value_rows,
    out_gate,
    in_gate,
    forget_gate,
    out_proj,
    ffn_gain,
    gate_proj,
    up_proj,
    down_proj,
    expert_ids,
    route_weights,
):
    total, mine = lax.axis_size("sp"), lax.axis_index("sp")
    groups = total // GROUP
    rows, width = stream.shape
    choices = expert_ids.shape[1]
    capacity = 2 * choices * rows // total
    cores = lax.axis_size("tp")

    def to_group(value, step):
        pairs = [
            (s, ((s // GROUP + step) % groups) * GROUP + (s % GROUP ^ ACROSS)) for s in range(total)
        ]
        return lax.ppermute(value, "sp", pairs)

    def other_core(value, step):
        return lax.ppermute(value, "tp", [(c, (c + step) % cores) for c in range(cores)])

    halves = [(gate_proj[0], up_proj[0], down_proj[0])] + [
        tuple(other_core(w[0], step) for w in (gate_proj, up_proj, down_proj))
        for step in range(1, cores)
    ]
    ids = [expert_ids] + [to_group(expert_ids, step) for step in range(1, groups)]
    shares = [route_weights] + [to_group(route_weights, step) for step in range(1, groups)]
    first = (mine // GROUP) * GROUP
    slot_count = GROUP * capacity
    places, backs = [], []
    for ids_one, share in zip(ids, shares):
        slot = slots_of(ids_one, first, capacity)
        here = jnp.arange(slot_count)
        places.append(
            sum((slot[:, j][None, :] == here[:, None]).astype(bf16) for j in range(choices))
        )
        backs.append(
            sum(
                jnp.where(slot[:, j][:, None] == here[None, :], share[:, j][:, None], 0.0)
                for j in range(choices)
            ).astype(bf16)
        )

    heads_out = mixer(queries, key_rows, value_rows, out_gate, in_gate, forget_gate)
    features = heads_out.shape[1]
    (token_heads,) = exchange(
        (heads_out.reshape(cores, rows, features),), ("slab",), "tp", cores, 3, 2_000_000
    )
    mix = sum(
        jnp.dot(token_heads[c], out_proj[c * features : (c + 1) * features], preferred_element_type=f32)
        for c in range(cores)
    )
    middle = (stream.astype(f32) + mix).astype(bf16)
    middle_float = middle.astype(f32)
    normed = (
        middle_float
        * lax.rsqrt(jnp.mean(middle_float * middle_float, axis=-1, keepdims=True) + epsilon)
        * ffn_gain
    ).astype(bf16)

    arrays = (normed, middle, jnp.stack(places), jnp.stack(backs))
    return expert_layer(arrays, [w for half in halves for w in half], groups, capacity)


def solution(mesh):
    in_specs = (
        P(("sp", "tp"), None),
        P("sp", "tp"),
        P("sp", "tp"),
        P("sp", "tp"),
        P("sp", "tp"),
        P("tp", "sp"),
        P("tp", "sp"),
        P(),
        P(),
        P("sp", None, "tp"),
        P("sp", None, "tp"),
        P("sp", "tp", None),
        P(("sp", "tp"), None),
        P(("sp", "tp"), None),
    )
    out_specs = P(("sp", "tp"), None)
    return jax.shard_map(body, mesh=mesh, in_specs=in_specs, out_specs=out_specs, check_vma=False)
```
